512 devices in a mesh: fs: 64 (over z, y), tp: 8 (over x, core).
Axes of the slice: x: 4, y: 4, z: 16, core: 2. Of those that a mesh axis runs over, the one named last changes fastest.
Arguments:
- tokens: bfloat16 [16384, 2048], P('fs', 'tp'), may hold values from -16 to 16, as said below
- mix_gain: bfloat16 [2048], P('tp'), may hold values from 0.099609375 to 1.8984375
- query_weight: bfloat16 [2048, 512], P('fs', 'tp'), may hold values from -0.125 to 0.125
- key_weight: bfloat16 [2048, 512], P('fs', 'tp'), may hold values from -0.125 to 0.125
- value_weight: bfloat16 [2048, 1024], P('fs', 'tp'), may hold values from -0.125 to 0.125
- output_gate_weight: bfloat16 [2048, 1024], P('fs', 'tp'), may hold values from -0.125 to 0.125
- out_weight: bfloat16 [1024, 2048], P('tp', 'fs'), may hold values from -0.1875 to 0.1875
- head_rates: float32 [8], P('tp'), may hold values from 0 to 1, as said below
- block_scale: float32 [128], P('fs'), may hold values from 0.5 to 2
- ffn_gain: bfloat16 [2048], P('tp'), may hold values from 0.099609375 to 1.8984375
- ff_gate: bfloat16 [2048, 5632], P('fs', 'tp'), may hold values from -0.125 to 0.125
- ff_up: bfloat16 [2048, 5632], P('fs', 'tp'), may hold values from -0.125 to 0.125
- ff_down: bfloat16 [5632, 2048], P('tp', 'fs'), may hold values from -0.078125 to 0.078125
- final_gain: bfloat16 [2048], P('tp'), may hold values from 0.099609375 to 1.8984375
Outputs:
- layer_out: bfloat16 [16384, 2048], P('fs', 'tp')
The draws below stay inside these ranges and needn't reach their ends.
Inputs may be any that keep to these rules, and one draw needn't show every extreme that they name: `tokens`: column blocks of the activations have different scales. `head_rates`: positive rates.
All inputs are finite; a program needn't handle non-finite values.
Results may differ from the reference program's by a relative error of at most 0.014.
Values may be sent and summed in bfloat16 or wider, within the bound.
A program may use at most 64 MiB of HBM per device.

```python
import math
import jax
import jax.numpy as jnp
from jax import lax

D = 2048
HEADS = 8
DK = 64
DV = 128
FF = 5632
BLK = 128
SEQ_LEN = 256
TOKENS = 16384
N_TP = 8


def draw_tokens(key, part):
    first, second, third = jax.random.split(jax.random.fold_in(key, 11), 3)
    groups = 2 * N_TP
    scales = jnp.exp(jax.random.uniform(second, (groups,), jnp.float32, -1.2, 1.2))
    base = jnp.clip(jax.random.normal(first, (TOKENS, D), jnp.float32), -4.0, 4.0)
    shaped = base.reshape(TOKENS, groups, D // groups) * scales[None, :, None]
    return shaped.reshape(TOKENS, D).astype(jnp.bfloat16)


def draw_head_rates(key, part):
    first, second, third = jax.random.split(jax.random.fold_in(key, 23), 3)
    fast = jax.random.uniform(first, (HEADS,), jnp.float32, 2.8, 4.3) / BLK
    slow = jax.random.uniform(second, (HEADS,), jnp.float32, 0.3, 1.0) / SEQ_LEN
    order = jax.random.permutation(third, HEADS)
    quick = order < HEADS // 2
    return jnp.where(quick, fast, slow).astype(jnp.float32)


def block_levels(own_key, dims, cuts, low, largest):
    level, own = 1.0, jax.random.fold_in(own_key, 6)
    for dim, parts in cuts:
        heights = jnp.exp(jax.random.uniform(jax.random.fold_in(own, dim), (parts,), jnp.float32, low / len(cuts), largest / len(cuts)))
        level = level * jnp.repeat(heights, dims[dim] // parts).reshape([-1 if axis == dim else 1 for axis in range(len(dims))])
    return level


def noise(rng, extent, scale, limit, shards=(), held_as=jnp.bfloat16):
    drawn = scale * jax.random.normal(rng, extent, jnp.float32)
    if shards:
        drawn = drawn * block_levels(rng, extent, shards, -0.22, 0.18)
    return jnp.clip(drawn, -limit, limit).astype(held_as)


def setup_inputs(seed: int = 0) -> dict:
    seeds = jax.random.split(jax.random.key(seed), 15)
    tokens = draw_tokens(jax.random.fold_in(seeds[14], 71), 0)
    mix_gain = jnp.clip(1.0 + 0.18 * jax.random.normal(seeds[1], (D,), jnp.float32), 0.099609375, 1.8984375).astype(jnp.bfloat16)
    query_weight = noise(seeds[2], (D, HEADS * DK), D ** -0.5, 0.125, ((0, 64), (1, 8)))
    key_weight = noise(seeds[3], (D, HEADS * DK), D ** -0.5, 0.125, ((0, 64), (1, 8)))
    value_weight = noise(seeds[4], (D, HEADS * DV), D ** -0.5, 0.125, ((0, 64), (1, 8)))
    output_gate_weight = noise(seeds[5], (D, HEADS * DV), D ** -0.5, 0.125, ((0, 64), (1, 8)))
    out_weight = noise(seeds[6], (HEADS * DV, D), (HEADS * DV) ** -0.5, 0.1875, ((0, 8), (1, 64)))
    head_rates = draw_head_rates(jax.random.fold_in(seeds[14], 71), 0)
    block_scale = jnp.clip(jnp.exp(math.log(2.0) - 1.3862944 * jax.random.uniform(seeds[8], (TOKENS // BLK,), jnp.float32) ** block_levels(seeds[8], (TOKENS // BLK,), ((0, 64),), -0.2, 0.2)), 0.5, 2.0)
    ffn_gain = jnp.clip(1.0 + 0.18 * jax.random.normal(seeds[9], (D,), jnp.float32), 0.099609375, 1.8984375).astype(jnp.bfloat16)
    ff_gate = noise(seeds[10], (D, FF), D ** -0.5, 0.125, ((0, 64), (1, 8)))
    ff_up = noise(seeds[11], (D, FF), D ** -0.5, 0.125, ((0, 64), (1, 8)))
    ff_down = noise(seeds[12], (FF, D), FF ** -0.5, 0.078125, ((0, 8), (1, 64)))
    final_gain = jnp.clip(1.0 + 0.18 * jax.random.normal(seeds[13], (D,), jnp.float32), 0.099609375, 1.8984375).astype(jnp.bfloat16)
    return dict(tokens=tokens, mix_gain=mix_gain, query_weight=query_weight, key_weight=key_weight, value_weight=value_weight, output_gate_weight=output_gate_weight, out_weight=out_weight, head_rates=head_rates, block_scale=block_scale, ffn_gain=ffn_gain, ff_gate=ff_gate, ff_up=ff_up, ff_down=ff_down, final_gain=final_gain)


EPS = 1e-06
THETA = 10000.0

def rms_norm(values, gain):
    scale = lax.rsqrt(lax.optimization_barrier(jnp.mean(values * values, axis=-1, keepdims=True)) + EPS)
    return values * scale * gain.astype(jnp.float32)

def rotate(values, positions):
    half = values.shape[-1] // 2
    inverse = THETA ** (-jnp.arange(half, dtype=jnp.float32) / half)
    angle = positions.astype(jnp.float32)[:, None] * inverse
    cosine = jnp.cos(angle)[:, None, :]
    sine = jnp.sin(angle)[:, None, :]
    first = values[..., :half]
    second = values[..., half:]
    return jnp.concatenate([first * cosine - second * sine, second * cosine + first * sine], axis=-1)

def retain(query, key, value, rates, scales):
    rows, heads_here, width_k = query.shape
    width_v = value.shape[-1]
    nblk = rows // BLK
    hi = lax.Precision.HIGHEST
    qblk = query.astype(jnp.float32).reshape(nblk, BLK, heads_here, width_k)
    kblk = key.astype(jnp.float32).reshape(nblk, BLK, heads_here, width_k)
    vblk = value.astype(jnp.float32).reshape(nblk, BLK, heads_here, width_v)
    logdec = -rates[None, :] * scales[:, None]
    steps = jnp.arange(BLK, dtype=jnp.float32)
    offset = steps[:, None] - steps[None, :]
    causal = offset >= 0
    inside = jnp.where(causal[None, None], jnp.exp(logdec[:, :, None, None] * jnp.where(causal, offset, 0.0)[None, None]), 0.0)
    scores = jnp.einsum('nchd,nmhd->nhcm', qblk, kblk, precision=hi) * inside
    inner = jnp.einsum('nhcm,nmhe->nche', scores, vblk, precision=hi)
    zeta = jnp.exp(logdec[:, :, None] * (BLK - 1.0 - steps)[None, None, :])
    kv_block = jnp.einsum('nchd,nche->nhde', kblk * jnp.transpose(zeta, (0, 2, 1))[..., None], vblk, precision=hi)
    hold = jnp.exp(logdec * BLK)
    per_seq = SEQ_LEN // BLK
    fresh = (jnp.arange(nblk, dtype=jnp.int32) % per_seq == 0).astype(jnp.float32)

    def advance(state, inputs):
        kv_now, hold_now, fresh_now = inputs
        before = state * (1.0 - fresh_now)
        return (before * hold_now[:, None, None] + kv_now, before)
    start = jnp.zeros((heads_here, width_k, width_v), jnp.float32)
    _, before = lax.scan(advance, start, (kv_block, hold, fresh))
    xi = jnp.exp(logdec[:, :, None] * (steps + 1.0)[None, None, :])
    cross = jnp.einsum('nchd,nhde->nche', qblk * jnp.transpose(xi, (0, 2, 1))[..., None], before, precision=hi)
    total = inner + cross
    total = total * lax.rsqrt(lax.optimization_barrier(jnp.mean(total * total, axis=-1, keepdims=True)) + EPS)
    return total.reshape(rows, heads_here, width_v)

def grouped_product(left, right, groups):
    width = left.shape[1] // groups
    result = jnp.zeros((left.shape[0], right.shape[1]), jnp.float32)
    for index in range(groups):
        partial_sum = jnp.dot(left[:, index * width:(index + 1) * width], right[index * width:(index + 1) * width], preferred_element_type=jnp.float32)
        result = result + partial_sum.astype(jnp.bfloat16).astype(jnp.float32)
    return result

def reference(tokens, mix_gain, query_weight, key_weight, value_weight, output_gate_weight, out_weight, head_rates, block_scale, ffn_gain, ff_gate, ff_up, ff_down, final_gain):
    rows = tokens.shape[0]
    positions = jnp.arange(rows, dtype=jnp.int32) % SEQ_LEN
    normed = rms_norm(tokens.astype(jnp.float32), mix_gain).astype(jnp.bfloat16)
    qproj = jnp.dot(normed, query_weight, preferred_element_type=jnp.float32).reshape(rows, HEADS, DK)
    kproj = jnp.dot(normed, key_weight, preferred_element_type=jnp.float32).reshape(rows, HEADS, DK)
    vproj = jnp.dot(normed, value_weight, preferred_element_type=jnp.float32)
    gproj = jnp.dot(normed, output_gate_weight, preferred_element_type=jnp.float32)
    query = rotate(qproj, positions).astype(jnp.bfloat16)
    key = (rotate(kproj, positions) * DK ** (-0.5)).astype(jnp.bfloat16)
    value = vproj.astype(jnp.bfloat16).reshape(rows, HEADS, DV)
    normret = retain(query, key, value, head_rates, block_scale).reshape(rows, HEADS * DV)
    gated = (normret * jax.nn.silu(gproj)).astype(jnp.bfloat16)
    mix = grouped_product(gated, out_weight, N_TP)
    resid = (tokens.astype(jnp.float32) + mix).astype(jnp.bfloat16)
    normed2 = rms_norm(resid.astype(jnp.float32), ffn_gain).astype(jnp.bfloat16)
    gate_part = jnp.dot(normed2, ff_gate, preferred_element_type=jnp.float32)
    up_part = jnp.dot(normed2, ff_up, preferred_element_type=jnp.float32)
    hidden = (jax.nn.silu(gate_part) * up_part).astype(jnp.bfloat16)
    ffn = grouped_product(hidden, ff_down, N_TP)
    total = resid.astype(jnp.float32) + ffn
    return rms_norm(total, final_gain).astype(jnp.bfloat16)
```

```python
import jax
import jax.numpy as jnp
import numpy as np
from jax import lax
from jax.experimental import pallas as pl
from jax.experimental.pallas import tpu as pltpu
from jax.sharding import PartitionSpec as P

MESH = pl.DeviceIdType.MESH
F32 = jnp.float32
BF16 = jnp.bfloat16
EPS = 1e-06
THETA = 10000.0
D = 2048
DK = 64
BLK = 128
SEQ = 256
Z, Y, X, C = 16, 4, 4, 2
HID = 176
NT = (((1,), (1,)), ((), ()))
N_SEND, N_RECV = 110, 170


def dot(a, b):
    return jnp.dot(a, b, preferred_element_type=F32)


def dot_nt(a, b):
    return lax.dot_general(a, b, NT, preferred_element_type=F32)


def iota(shape, dim):
    return lax.broadcasted_iota(jnp.int32, shape, dim)


def copy_to(src, dst, send, recv, where):
    return pltpu.make_async_remote_copy(
        src_ref=src, dst_ref=dst, send_sem=send, recv_sem=recv, device_id=where, device_id_type=MESH
    )


def wait_bytes(ref, sem):
    pltpu.make_async_copy(ref, ref, sem).wait()


def kernel(
    tok, mix_gain, qw, kw, vw, gw, ow, rates, scales, ffn_gain, ffg, ffu, ffd, fin, cos, sin,
    out,
    wq, slab, a2a, ffw, xt, xn, wo, gat, res, x2, part, sib, r1, r2, r3, r4, stat, stats,
    ssem, rsem, zsend, ysend, fsend, yshare,
):
    fs, tp = lax.axis_index("fs"), lax.axis_index("tp")
    z, y = fs // Y, fs % Y
    x, c = tp // C, tp % C
    o = 1 - c
    zr, zl = (z + 1) % Z, (z + Z - 1) % Z
    yp, y2, ym = (y + 1) % Y, (y + 2) % Y, (y + 3) % Y
    xp, xo, xm = (x + 1) % X, (x + 2) % X, (x + 3) % X

    def at(zz=z, yy=y, xx=x, cc=c):
        return (zz * Y + yy, xx * C + cc)

    used = [0, 0]
    pending = []

    def fresh():
        used[1] += 1
        return rsem.at[used[1] - 1]

    def send(src, dst, recv, where):
        used[0] += 1
        copy = copy_to(src, dst, ssem.at[used[0] - 1], recv, where)
        copy.start()
        pending.append(copy)
        return copy

    class Ring4:
        def __init__(self, slab_of, me, prev, nxt, to_prev, to_next):
            self.slab, self.me, self.prev, self.nxt = slab_of, me, prev, nxt
            self.to_prev, self.to_next = to_prev, to_next
            self.sems = [fresh() for _ in range(4)]

        def start(self):
            s = self.slab(self.me)
            self.a = send(s, s, self.sems[0], self.to_next)
            self.b = send(s, s, self.sems[1], self.to_prev)

        def relay(self):
            self.a.wait_recv()
            s = self.slab(self.prev, 0)
            self.d = send(s, s, self.sems[2], self.to_next)
            self.b.wait_recv()
            s = self.slab(self.nxt, 1)
            self.e = send(s, s, self.sems[3], self.to_prev)

        def finish(self):
            self.d.wait_recv()
            self.e.wait_recv()

    row0 = pl.multiple_of(z * (Y * 32) + y * 32, 32)
    e0 = (iota((64, 128), 0) == iota((64, 128), 1)).astype(BF16)
    e1 = (iota((64, 128), 0) + 64 == iota((64, 128), 1)).astype(BF16)
    i32 = (iota((32, 32), 0) == iota((32, 32), 1)).astype(BF16)
    wq[pl.ds(row0, 32), 0:128] = (dot(qw[...], e0) + dot(kw[...], e1)).astype(BF16)
    wq[pl.ds(row0, 32), 128:256] = vw[...]
    wq[pl.ds(row0, 32), 256:384] = gw[...]
    wq[pl.ds(row0, 32), 384:512] = dot_nt(i32, ow[...]).astype(BF16)
    xt[c, x, 0:256, :] = tok[...]
    xt[c, x, 256:272, :] = jnp.concatenate(
        [jnp.broadcast_to(mix_gain[...], (8, 256)), jnp.broadcast_to(ffn_gain[...], (8, 256))], axis=0
    )
    gt = ffg[...].astype(F32)
    ut = ffu[...].astype(F32)
    zero = jnp.zeros((32, 704), F32)
    tall = jnp.concatenate([gt, ut, zero, zero], axis=0)
    tall = jnp.concatenate([tall, jnp.zeros((128, 64), F32)], axis=1)
    turned = tall.T
    ed = (iota((32, 128), 0) + 64 == iota((32, 128), 1)).astype(BF16)
    slab[...] = (turned[0:704, :] + dot(ffd[...], ed)).astype(BF16)

    barrier = pltpu.get_barrier_semaphore()
    partners = [at(zz=zr), at(zz=zl), at(yy=yp), at(yy=y2), at(yy=ym)]
    partners += [at(xx=xx, cc=cc) for xx in (x, xp, xo, xm) for cc in (c, o)][1:]
    for who in partners:
        pl.semaphore_signal(barrier, inc=1, device_id=who, device_id_type=MESH)
    pl.semaphore_wait(barrier, len(partners))

    def wblk(zz, yy):
        return wq.at[pl.ds(pl.multiple_of(zz * (Y * 32) + yy * 32, 32), 32), :]

    left_sem = [fresh() for _ in range(8)]
    right_sem = [fresh() for _ in range(7)]
    yleft = [fresh() for _ in range(9)]
    yright = [fresh() for _ in range(7)]

    def z_send(zz, sem, where):
        copy_to(wblk(zz, y), wblk(zz, y), zsend, sem, where).start()

    def y_send(zz, yy, sem, where):
        copy_to(wblk(zz, yy), wblk(zz, yy), ysend, sem, where).start()

    def serve_w(s):
        if s == 0:
            z_send(z, left_sem[0], at(zz=zr))
            z_send(z, right_sem[0], at(zz=zl))
            y_send(z, y, yleft[0], at(yy=yp))
            y_send(z, y, yshare.at[1], at(yy=ym))
            return
        if s <= 8:
            zz = (z + Z - s) % Z
            copy_to(wblk(zz, y), wblk(zz, y), zsend, left_sem[s - 1], at(zz=zr)).wait_recv()
            if s < 8:
                z_send(zz, left_sem[s], at(zz=zr))
            y_send(zz, y, yleft[s], at(yy=yp))
            y_send(zz, y, yshare.at[1], at(yy=ym))
        if s <= 7:
            zz = (z + s) % Z
            copy_to(wblk(zz, y), wblk(zz, y), zsend, right_sem[s - 1], at(zz=zl)).wait_recv()
            if s < 7:
                z_send(zz, right_sem[s], at(zz=zl))
            y_send(zz, y, yright[s - 1], at(yy=ym))
            y_send(zz, y, yshare.at[0], at(yy=yp))

    def relay_y(s):
        zz = (z + Z - s) % Z
        copy_to(wblk(zz, ym), wblk(zz, ym), ysend, yleft[s], at(yy=yp)).wait_recv()
        y_send(zz, ym, yshare.at[2], at(yy=yp))
        if 1 <= s <= 7:
            zz = (z + s) % Z
            copy_to(wblk(zz, yp), wblk(zz, yp), ysend, yright[s - 1], at(yy=ym)).wait_recv()
            y_send(zz, yp, yshare.at[3], at(yy=ym))

    groups = ((0, 1), (1, 3))
    fleft = [[fresh() for _ in range(8)] for _ in groups]
    fright = [[fresh() for _ in range(7)] for _ in groups]

    def fblk(g, zz):
        lo, hi = groups[g]
        return ffw.at[lo:hi, :, pl.ds(pl.multiple_of(zz * 128, 128), 128)]

    def f_send(g, zz, sem, where):
        copy_to(fblk(g, zz), fblk(g, zz), fsend.at[g], sem, where).start()

    def serve_f(g, s):
        if s == 0:
            f_send(g, z, fleft[g][0], at(zz=zr))
            f_send(g, z, fright[g][0], at(zz=zl))
            return
        zz = (z + Z - s) % Z
        copy_to(fblk(g, zz), fblk(g, zz), fsend.at[g], fleft[g][s - 1], at(zz=zr)).wait_recv()
        if s < 8:
            f_send(g, zz, fleft[g][s], at(zz=zr))
        if s <= 7:
            zz = (z + s) % Z
            copy_to(fblk(g, zz), fblk(g, zz), fsend.at[g], fright[g][s - 1], at(zz=zl)).wait_recv()
            if s < 7:
                f_send(g, zz, fright[g][s], at(zz=zl))

    serve_w(0)

    def to_sibling(ref, sem):
        return send(ref, ref, sem, at(cc=o))

    tok_ring = Ring4(
        lambda j, half=None: xt.at[c, j, (slice(0, 272), slice(0, 144), slice(144, 272))[0 if half is None else half + 1], :],
        x, xm, xp, at(xx=xm), at(xx=xp),
    )
    tok_ring.start()
    tok_sib = [to_sibling(xt.at[c, x], fresh())]
    a2a_copies = []
    for yy in (yp, y2, ym):
        a2a_copies.append(
            send(slab.at[pl.ds(pl.multiple_of(yy * HID, 16), HID), :], a2a.at[y], fresh(), at(yy=yy))
        )
    serve_w(1)
    tok_ring.relay()
    tok_sib += [to_sibling(xt.at[c, xm], fresh()), to_sibling(xt.at[c, xp], fresh())]
    relay_y(0)
    for copy in a2a_copies:
        copy.wait_recv()

    pick = jnp.zeros((HID, 384), F32)
    ln, col = iota((128, 384), 0), iota((128, 384), 1)
    same = (ln // 32 == col // 128) & (ln % 32 == col % 32)
    own = slab[pl.ds(pl.multiple_of(y * HID, 16), HID), :]
    for yy in range(Y):
        chosen = (same & ((col % 128) // 32 == yy)).astype(BF16)
        pick = pick + dot(jnp.where(yy == y, own, a2a[yy]), chosen)
    zlane = pl.ds(pl.multiple_of(z * 128, 128), 128)
    for p in range(3):
        ffw[p, :, zlane] = pick[:, p * 128 : (p + 1) * 128].astype(BF16)

    serve_w(2)
    relay_y(1)
    serve_f(0, 0)
    tok_ring.finish()
    tok_sib.append(to_sibling(xt.at[c, xo], fresh()))
    serve_w(3)
    relay_y(2)
    serve_f(0, 1)
    serve_f(1, 0)
    for copy in tok_sib:
        copy.wait_recv()

    total = jnp.zeros((SEQ, 1), F32)
    for t in range(8):
        v = xt[t % 2, t // 2, 0:256, :].astype(F32)
        total = total + jnp.sum(v * v, axis=1, keepdims=True)
    scale = lax.rsqrt(total * (1.0 / D) + EPS)
    for t in range(8):
        v = xt[t % 2, t // 2, 0:256, :].astype(F32)
        g = xt[t % 2, t // 2, 256:257, :].astype(F32)
        xn[:, t * 256 : (t + 1) * 256] = (v * scale * g).astype(BF16)

    for s in range(4, 9):
        serve_w(s)
        relay_y(s - 1)
        serve_f(0, s - 2)
    relay_y(8)
    wait_bytes(wq.at[0 : 7 * 32], yshare.at[0])
    wait_bytes(wq.at[0 : 9 * 32], yshare.at[1])
    wait_bytes(wq.at[0 : 9 * 32], yshare.at[2])
    wait_bytes(wq.at[0 : 7 * 32], yshare.at[3])

    def wo_src(t):
        return wq.at[pl.ds(pl.multiple_of(t * 256, 256), 256), 384:512]

    wo_copies = []
    for xx, cc in [(xx, cc) for xx in (x, xp, xo, xm) for cc in (c, o)][1:]:
        wo_copies.append(send(wo_src(xx * C + cc), wo.at[c, x], fresh(), at(xx=xx, cc=cc)))
    wo[c, x] = wq[pl.ds(pl.multiple_of(tp * 256, 256), 256), 384:512]

    proj = dot(xn[...], wq[:, 0:384])
    serve_f(0, 7)
    serve_f(0, 8)
    serve_f(1, 1)

    qk = proj[:, 0:128]
    lane = iota((SEQ, 128), 1)
    swapped = jnp.where(lane % 64 < 32, pltpu.roll(qk, 96, 1), pltpu.roll(qk, 32, 1))
    turned_qk = qk * cos[...] + swapped * sin[...]
    query = jnp.where(lane < 64, turned_qk, 0.0).astype(BF16)
    key = pltpu.roll(turned_qk, 64, 1).astype(BF16)
    value = proj[:, 128:256].astype(BF16)
    later, earlier = iota((SEQ, SEQ), 0), iota((SEQ, SEQ), 1)
    n0 = jnp.minimum(later, BLK - 1) - jnp.minimum(earlier, BLK - 1)
    n1 = jnp.maximum(later, BLK - 1) - jnp.maximum(earlier, BLK - 1)
    rate = rates[0]
    power = n0.astype(F32) * (-rate * scales[0]) + n1.astype(F32) * (-rate * scales[1])
    causal = later >= earlier
    inside = jnp.where(causal, jnp.exp(jnp.where(causal, power, 0.0)), 0.0)
    scores = dot_nt(query, key) * inside
    high = scores.astype(BF16)
    low = (scores - high.astype(F32)).astype(BF16)
    ret = dot(high, value) + dot(low, value)
    ret = ret * lax.rsqrt(jnp.mean(ret * ret, axis=1, keepdims=True) + EPS)
    g = proj[:, 256:384]
    gat[c, x] = (ret * (g * jax.nn.sigmoid(g))).astype(BF16)
    serve_f(1, 2)
    gat_ring = Ring4(
        lambda j, half=None: gat.at[c, j, (slice(0, 256), slice(0, 128), slice(128, 256))[0 if half is None else half + 1], :],
        x, xm, xp, at(xx=xm), at(xx=xp),
    )
    gat_ring.start()
    gat_sib = [to_sibling(gat.at[c, x], fresh())]
    gat_ring.relay()
    gat_sib += [to_sibling(gat.at[c, xm], fresh()), to_sibling(gat.at[c, xp], fresh())]
    serve_f(1, 3)
    gat_ring.finish()
    gat_sib.append(to_sibling(gat.at[c, xo], fresh()))
    for copy in wo_copies:
        copy.wait_recv()
    for copy in gat_sib:
        copy.wait_recv()
    mix = jnp.zeros((SEQ, 256), F32)
    for t in range(8):
        term = dot_nt(gat[t % 2, t // 2], wo[t % 2, t // 2])
        mix = mix + term.astype(BF16).astype(F32)
    resid = (tok[...].astype(F32) + mix).astype(BF16)
    res[...] = resid
    x2[c, y, x] = resid
    serve_f(1, 4)

    A, B = slice(0, 128), slice(128, 256)

    def pair(half):
        return slice(0, 4) if half is None else slice(2 * half, 2 * half + 2)

    def rows(base, half):
        return slice(base, base + 128) if half is None else slice(base + 64 * half, base + 64 * half + 64)

    toy, tox = (at(yy=ym), at(yy=yp)), (at(xx=xm), at(xx=xp))
    ring_a1 = Ring4(lambda j, half=None: x2.at[c, y, j, rows(0, half), :], x, xm, xp, *tox)
    ring_b1 = Ring4(lambda j, half=None: x2.at[c, j, x, rows(128, half), :], y, ym, yp, *toy)
    ring_a2 = Ring4(lambda j, half=None: x2.at[c, j, pair(half), A, :], y, ym, yp, *toy)
    ring_b2 = Ring4(lambda j, half=None: x2.at[c, pair(half), j, B, :], x, xm, xp, *tox)
    ring_a1.start()
    ring_b1.start()
    ring_a1.relay()
    ring_b1.relay()
    serve_f(1, 5)
    ring_a1.finish()
    ring_a2.start()
    ring_b1.finish()
    ring_b2.start()
    x2_sib = [to_sibling(x2.at[c, y, :, A, :], fresh()), to_sibling(x2.at[c, :, x, B, :], fresh())]
    serve_f(1, 6)
    ring_a2.relay()
    ring_b2.relay()
    for yy, xx in ((ym, xm), (yp, xp)):
        x2_sib += [to_sibling(x2.at[c, yy, :, A, :], fresh()), to_sibling(x2.at[c, :, xx, B, :], fresh())]
    serve_f(1, 7)
    serve_f(1, 8)
    ring_a2.finish()
    ring_b2.finish()
    x2_sib += [to_sibling(x2.at[c, y2, :, A, :], fresh()), to_sibling(x2.at[c, :, xo, B, :], fresh())]
    for copy in x2_sib:
        copy.wait_recv()

    part_sem = [fresh() for _ in range(Y)]
    part_copies = []
    for s in range(Y):
        total = jnp.zeros((SEQ, 1), F32)
        for t in range(8):
            v = x2[t % 2, s, t // 2].astype(F32)
            total = total + jnp.sum(v * v, axis=1, keepdims=True)
        scale = lax.rsqrt(total * (1.0 / D) + EPS)
        for t in range(8):
            v = x2[t % 2, s, t // 2].astype(F32)
            g = xt[t % 2, t // 2, 264:265, :].astype(F32)
            xn[:, t * 256 : (t + 1) * 256] = (v * scale * g).astype(BF16)
        gate = dot_nt(xn[...], ffw[0])
        up = dot_nt(xn[...], ffw[1])
        hidden = (gate * jax.nn.sigmoid(gate) * up).astype(BF16)
        for cc in (o, c):
            for xx in range(X):
                lanes = pl.ds(pl.multiple_of((xx * C + cc) * 256, 256), 256)
                part[cc, s, xx] = dot(hidden, ffw[2, :, lanes]).astype(BF16)
            if cc is o:
                part_copies.append(send(part.at[o, s], sib.at[s], part_sem[s], at(cc=o)))
    for s in range(Y):
        part_copies[s].wait_recv()
        part[c, s] = part[c, s] + sib[s]

    class Sum4:
        def __init__(self, slab_of, first, second, me, prev, nxt, opp, to_prev, to_next):
            self.slab, self.first, self.second = slab_of, first, second
            self.me, self.prev, self.nxt, self.opp = me, prev, nxt, opp
            self.to_prev, self.to_next = to_prev, to_next
            self.sems = [fresh() for _ in range(4)]

        def start(self):
            self.a = send(self.slab(self.opp, 0), self.first.at[0], self.sems[0], self.to_next)
            self.b = send(self.slab(self.opp, 1), self.first.at[1], self.sems[1], self.to_prev)

        def middle(self):
            self.a.wait_recv()
            ref = self.slab(self.nxt, 0)
            ref[...] = ref[...] + self.first[0]
            self.b.wait_recv()
            ref = self.slab(self.prev, 1)
            ref[...] = ref[...] + self.first[1]
            self.d = send(self.slab(self.nxt), self.second.at[0], self.sems[2], self.to_next)
            self.e = send(self.slab(self.prev), self.second.at[1], self.sems[3], self.to_prev)

        def finish(self):
            self.d.wait_recv()
            self.e.wait_recv()

    sum_a1 = Sum4(lambda j, half=None: part.at[c, j, pair(half), A, :], r1.at[0], r2.at[0], y, ym, yp, y2, *toy)
    sum_b1 = Sum4(lambda j, half=None: part.at[c, pair(half), j, B, :], r1.at[1], r2.at[1], x, xm, xp, xo, *tox)
    sum_a2 = Sum4(lambda j, half=None: part.at[c, y, j, rows(0, half), :], r3.at[0], r4.at[0], x, xm, xp, xo, *tox)
    sum_b2 = Sum4(lambda j, half=None: part.at[c, j, x, rows(128, half), :], r3.at[1], r4.at[1], y, ym, yp, y2, *toy)
    sum_a1.start()
    sum_b1.start()
    sum_a1.middle()
    sum_b1.middle()
    sum_a1.finish()
    for xx in range(X):
        mine = part[c, y, xx, A, :].astype(F32) + r2[0, 0, xx].astype(F32) + r2[0, 1, xx].astype(F32)
        part[c, y, xx, A, :] = mine.astype(BF16)
    sum_a2.start()
    sum_b1.finish()
    for yy in range(Y):
        mine = part[c, yy, x, B, :].astype(F32) + r2[1, 0, yy].astype(F32) + r2[1, 1, yy].astype(F32)
        part[c, yy, x, B, :] = mine.astype(BF16)
    sum_b2.start()
    sum_a2.middle()
    sum_b2.middle()
    sum_a2.finish()
    sum_b2.finish()
    ffn = jnp.concatenate(
        [r4[h, 0].astype(F32) + r4[h, 1].astype(F32) for h in range(2)], axis=0
    ) + part[c, y, x].astype(F32)
    total = res[...].astype(F32) + ffn

    squares = jnp.sum(total * total, axis=1, keepdims=True)
    turned = jnp.broadcast_to(squares, (SEQ, 128)).T
    stat[...] = turned[0:8, :]
    stat_copies = []
    for xx, cc in [(xx, cc) for xx in (x, xp, xo, xm) for cc in (c, o)][1:]:
        stat_copies.append(send(stat, stats.at[c, x], fresh(), at(xx=xx, cc=cc)))
    stats[c, x] = turned[0:8, :]
    for copy in stat_copies:
        copy.wait_recv()
    summed = stats[0, 0]
    for t in range(1, 8):
        summed = summed + stats[t % 2, t // 2]
    across = jnp.concatenate([summed] * 16, axis=0).T
    scale = lax.rsqrt(across * (1.0 / D) + EPS)
    out[:, 0:128] = (total[:, 0:128] * scale * fin[:, 0:128].astype(F32)).astype(BF16)
    out[:, 128:256] = (total[:, 128:256] * scale * fin[:, 128:256].astype(F32)).astype(BF16)

    for copy in pending:
        copy.wait_send()
    wait_bytes(wq.at[0 : 15 * 32], zsend)
    wait_bytes(wq.at[0 : 48 * 32], ysend)
    for g, (lo, hi) in enumerate(groups):
        wait_bytes(ffw.at[lo:hi, :, 0 : 15 * 128], fsend.at[g])
    assert used[0] <= N_SEND and used[1] <= N_RECV, used


def tables():
    half = DK // 2
    inverse = THETA ** (-np.arange(half, dtype=np.float64) / half)
    angle = np.arange(SEQ, dtype=np.float64)[:, None] * inverse
    cosine, sine = np.cos(angle), np.sin(angle)
    c1 = np.concatenate([cosine, cosine], axis=1)
    s1 = np.concatenate([-sine, sine], axis=1)
    k = DK ** (-0.5)
    return (
        np.concatenate([c1, c1 * k], axis=1).astype(np.float32),
        np.concatenate([s1, s1 * k], axis=1).astype(np.float32),
    )


def body(tokens, mix_gain, qw, kw, vw, gw, ow, rates, scales, ffn_gain, ffg, ffu, ffd, fin):
    cos, sin = tables()
    vmem = pl.BlockSpec(memory_space=pltpu.VMEM)
    smem = pl.BlockSpec(memory_space=pltpu.SMEM)
    return pl.pallas_call(
        kernel,
        name="layer",
        out_shape=jax.ShapeDtypeStruct((SEQ, 256), BF16),
        in_specs=[vmem] * 7 + [smem] * 2 + [vmem] * 7,
        out_specs=vmem,
        scratch_shapes=[
            pltpu.VMEM((D, 512), BF16),
            pltpu.VMEM((704, 128), BF16),
            pltpu.VMEM((Y, HID, 128), BF16),
            pltpu.VMEM((3, HID, D), BF16),
            pltpu.VMEM((C, X, 272, 256), BF16),
            pltpu.VMEM((SEQ, D), BF16),
            pltpu.VMEM((C, X, 256, 128), BF16),
            pltpu.VMEM((C, X, 256, 128), BF16),
            pltpu.VMEM((SEQ, 256), BF16),
            pltpu.VMEM((C, Y, X, 256, 256), BF16),
            pltpu.VMEM((C, Y, X, 256, 256), BF16),
            pltpu.VMEM((Y, X, 256, 256), BF16),
            pltpu.VMEM((2, 2, 2, 128, 256), BF16),
            pltpu.VMEM((2, 2, 4, 128, 256), BF16),
            pltpu.VMEM((2, 2, 64, 256), BF16),
            pltpu.VMEM((2, 2, 128, 256), BF16),
            pltpu.VMEM((8, SEQ), F32),
            pltpu.VMEM((C, X, 8, SEQ), F32),
            pltpu.SemaphoreType.DMA((N_SEND,)),
            pltpu.SemaphoreType.DMA((N_RECV,)),
            pltpu.SemaphoreType.DMA,
            pltpu.SemaphoreType.DMA,
            pltpu.SemaphoreType.DMA((2,)),
            pltpu.SemaphoreType.DMA((4,)),
        ],
        compiler_params=pltpu.CompilerParams(
            collective_id=0, has_side_effects=True, vmem_limit_bytes=60 * 1024 * 1024
        ),
    )(
        tokens, mix_gain.reshape(1, 256), qw, kw, vw, gw, ow, rates, scales,
        ffn_gain.reshape(1, 256), ffg, ffu, ffd, fin.reshape(1, 256),
        jnp.asarray(cos), jnp.asarray(sin),
    )


def solution(mesh):
    return jax.shard_map(
        body,
        mesh=mesh,
        in_specs=(
            P("fs", "tp"), P("tp"), P("fs", "tp"), P("fs", "tp"), P("fs", "tp"), P("fs", "tp"),
            P("tp", "fs"), P("tp"), P("fs"), P("tp"), P("fs", "tp"), P("fs", "tp"), P("tp", "fs"), P("tp"),
        ),
        out_specs=P("fs", "tp"),
        check_vma=False,
    )
```
